256 devices in a mesh: gr: 2 (over z_hi), fs: 16 (over z_lo, x), tp: 8 (over y, core).
Axes of the slice: x: 4, y: 4, z: 8 (z_hi: 2, z_lo: 4; z = z_hi * 4 + z_lo), core: 2. Of those that a mesh axis runs over, the one named last changes fastest.
Arguments:
- tokens: bfloat16 [6144, 4096], P(('gr', 'fs'), 'tp'), may hold values from -6 to 6
- route_ids: int32 [6144, 2], P(('gr', 'fs')), may hold values from 0 to 15, all different within a row; in each aligned block of 192 rows (0 to 191, 192 to 383, ...) at most 48 rows name the same one
- route_logits: float32 [6144, 2], P(('gr', 'fs')), may hold values from -6 to 6
- gain: float32 [4096], P(('gr', 'fs')), may hold values from 0.1 to 1.9
- gate_master: float32 [16, 4096, 2048], P(None, ('gr', 'fs'), 'tp'), may hold values from -6 to 6
- up_master: float32 [16, 4096, 2048], P(None, ('gr', 'fs'), 'tp'), may hold values from -6 to 6
- down_master: float32 [16, 2048, 4096], P(None, ('gr', 'fs'), 'tp'), may hold values from -6 to 6
Outputs:
- gate_weight: bfloat16 [16, 4096, 2048], P('fs', None, 'tp')
- up_weight: bfloat16 [16, 4096, 2048], P('fs', None, 'tp')
- down_weight: bfloat16 [16, 2048, 4096], P('fs', 'tp')
- mixed_out: bfloat16 [6144, 4096], P(('gr', 'fs'), 'tp')
The draws below stay inside these ranges and needn't reach their ends.
Inputs may be any that keep to these rules, and one draw needn't show every extreme that they name: `route_ids`: each row names 2 different experts; among the rows of one device no expert is named by more than 48 rows, a bound that some block reaches.
All inputs are finite; a program needn't handle non-finite values.
Results may differ from the reference program's by a relative error of at most 0.015.
Values may be sent and summed in bfloat16 or wider, within the bound.
No kernel may reach another device: no remote copies, remote signals or barrier semaphores. Data moves between devices by JAX's collectives and lax.ppermute only.
A program may use at most 128 MiB of HBM per device.

```python
import math
import jax
import jax.numpy as jnp
import numpy as np
from jax import lax

D = 4096
FF = 2048
TOP = 2
TOK_DEV = 192
EXPERTS = 16
CAP = 48
TOKENS = 6144
N_GR = 2
N_FS = 16
N_TP = 8


def levels(rng, extent, pieces, low, largest):
    def one(position, shards_of):
        draws = jax.random.uniform(jax.random.fold_in(jax.random.fold_in(rng, 6), position), (shards_of,), jnp.float32, low / len(pieces), largest / len(pieces))
        return jnp.repeat(jnp.exp(draws), extent[position] // shards_of).reshape((-1,) + (1,) * (len(extent) - position - 1))

    level = one(*pieces[0])
    for cut in pieces[1:]:
        level = level * one(*cut)
    return level


def deal_out(key, own, number, rows, number_of, top, most, skew):
    order = jax.random.permutation(key, number_of)
    packed, ordinary = portions_of(number_of, rows * top, most, skew, True), portions_of(number_of, rows * top, most, skew, False)
    places = jnp.arange(number_of)

    def named(tallies, offset_by):
        used = int((tallies > 0).sum())
        fixed = max(1, used // 4)
        passed = fixed + (places - fixed + offset_by * (used - fixed)) % max(1, number_of - fixed)
        return jnp.zeros((number_of,), jnp.int32).at[order[jnp.where(places < fixed, places, passed)]].set(jnp.asarray(tallies, jnp.int32))

    tallies = jnp.where(number % 4 == 0, named(packed, number // 4), named(ordinary, number - number // 4 - 1))
    mixed = jax.random.permutation(jax.random.fold_in(own, 3), number_of)
    source_of, taker = mixed[0:number_of // 2 * 2:2], mixed[1:number_of // 2 * 2:2]
    margin = jnp.minimum(tallies[source_of] - 1, most - tallies[taker]) // 2
    margin = jnp.where((source_of == order[0]) | (taker == order[0]) | (tallies[taker] == 0), 0, jnp.maximum(margin, 0))
    passed = jax.random.randint(jax.random.fold_in(own, 4), (number_of // 2,), 0, 1 << 20) % (margin + 1)
    tallies = tallies.at[source_of].add(-passed).at[taker].add(passed)
    items = jnp.searchsorted(jnp.cumsum(tallies), jnp.arange(rows * top), side="right").astype(jnp.int32)
    table = items.reshape(top, rows).T
    table = table[jax.random.permutation(jax.random.fold_in(own, 1), rows)]
    offset_by = jax.random.randint(jax.random.fold_in(own, 2), (rows, 1), 0, top)
    return jnp.take_along_axis(table, (jnp.arange(top)[None, :] + offset_by) % top, axis=1)


def portions_of(amount, total, bound, skew, full):
    weights = [(1 << 20) // math.isqrt(standing ** skew) + 1 for standing in range(1, amount + 1)]
    largest = bound if full else min(bound, max(-(-total // amount), total * weights[0] // sum(weights)))
    least = 1 if total - largest >= amount - 1 else 0
    given, spare = [largest] + [least] * (amount - 1), total - largest - least * (amount - 1)
    while spare > 0:
        candidates = [i for i in range(1, amount) if given[i] < largest] or [i for i in range(1, amount) if given[i] < bound]
        mass, remaining = sum([weights[i] for i in candidates]), spare
        for i in candidates:
            more = min(bound - given[i], max(1, remaining * weights[i] // mass), spare)
            given[i] = given[i] + more
            spare = spare - more
    return np.array(given)


def bell_draw(key, extent, spread, reach, shards=(), held_as=jnp.bfloat16):
    values = jax.random.normal(key, extent, jnp.float32) * spread
    if len(shards) > 0:
        values = levels(key, extent, shards, -0.22, 0.18) * values
    return jnp.clip(values, min=-reach, max=reach).astype(held_as)


def setup_inputs(seed: int = 0) -> dict:
    seeds = jax.random.split(jax.random.key(seed), 8)
    tokens = bell_draw(seeds[0], (TOKENS, D), 1.0, 6.0, ((0, 32), (1, 8)))
    route_ids_keys = jax.random.split(jax.random.fold_in(seeds[1], 1), TOKENS // TOK_DEV)
    route_ids_turns = jax.random.permutation(jax.random.fold_in(seeds[1], 3), TOKENS // TOK_DEV)
    route_ids = jax.vmap(lambda own, number: deal_out(jax.random.fold_in(seeds[1], 2), own, number, TOK_DEV, EXPERTS, TOP, CAP, 2))(route_ids_keys, route_ids_turns).reshape((TOKENS, TOP))
    route_logits = bell_draw(seeds[2], (TOKENS, TOP), 1.5, 6.0, ((0, 32),), jnp.float32)
    gain = jnp.clip(1.0 + 0.18 * jax.random.normal(seeds[3], (D,), jnp.float32), 0.1, 1.9)
    gate_master = bell_draw(seeds[4], (EXPERTS, D, FF), 1.0, 6.0, ((1, 32), (2, 8)), jnp.float32)
    up_master = bell_draw(seeds[5], (EXPERTS, D, FF), 1.0, 6.0, ((1, 32), (2, 8)), jnp.float32)
    down_master = bell_draw(seeds[6], (EXPERTS, FF, D), 1.0, 6.0, ((1, 32), (2, 8)), jnp.float32)
    return dict(tokens=tokens, route_ids=route_ids, route_logits=route_logits, gain=gain, gate_master=gate_master, up_master=up_master, down_master=down_master)


EPS = 1e-06

def reference(tokens, route_ids, route_logits, gain, gate_master, up_master, down_master):
    row_gain = gain[None, :, None]
    gate_weight = (gate_master * row_gain).astype(jnp.bfloat16)
    up_weight = (up_master * row_gain).astype(jnp.bfloat16)
    down_weight = down_master.astype(jnp.bfloat16)
    float_rows = tokens.astype(jnp.float32)
    normed = (float_rows * lax.rsqrt(lax.optimization_barrier(jnp.mean(float_rows * float_rows, axis=1, keepdims=True)) + EPS)).astype(jnp.bfloat16)
    sigmoid_vals = jax.nn.sigmoid(route_logits.astype(jnp.float32))
    shares = sigmoid_vals / lax.optimization_barrier(jnp.sum(sigmoid_vals, axis=1, keepdims=True))
    assign_count = TOKENS * TOP
    slot_limit = N_GR * N_FS * CAP
    flattened = route_ids.reshape(assign_count).astype(jnp.int32)
    sort_order = jnp.argsort(flattened).astype(jnp.int32)
    starts = jnp.searchsorted(flattened[sort_order], jnp.arange(EXPERTS, dtype=jnp.int32), side='left').astype(jnp.int32)
    padded_order = jnp.concatenate([sort_order, jnp.full((slot_limit,), assign_count, jnp.int32)])
    padded_ids = jnp.concatenate([flattened, jnp.full((1,), -1, jnp.int32)])
    padded_shares = jnp.concatenate([shares.reshape(assign_count), jnp.zeros((1,), jnp.float32)])
    padded_rows = jnp.concatenate([normed, jnp.zeros((1, D), jnp.bfloat16)], axis=0)

    def one_expert(expert):
        picked_index = lax.dynamic_slice_in_dim(padded_order, starts[expert], slot_limit)
        is_valid = padded_ids[picked_index] == expert
        token_index = jnp.where(is_valid, picked_index // TOP, TOKENS).astype(jnp.int32)
        expert_rows = padded_rows[token_index]
        gate_value = jnp.dot(expert_rows, gate_weight[expert], preferred_element_type=jnp.float32) * D ** (-0.5)
        up_value = jnp.dot(expert_rows, up_weight[expert], preferred_element_type=jnp.float32) * D ** (-0.5)
        hidden = (jax.nn.silu(gate_value) * up_value).astype(jnp.bfloat16)
        hidden_blocks = hidden.reshape(slot_limit, N_TP, FF // N_TP).astype(jnp.float32)
        down_blocks = down_weight[expert].reshape(N_TP, FF // N_TP, D).astype(jnp.float32)
        partials = jnp.einsum('mjf,jfd->jmd', hidden_blocks, down_blocks).astype(jnp.bfloat16)
        partials = lax.optimization_barrier(partials)
        expert_out = (lax.optimization_barrier(jnp.sum(partials.astype(jnp.float32), axis=0)) * FF ** (-0.5)).astype(jnp.bfloat16)
        expert_out = lax.optimization_barrier(expert_out)
        weights_here = jnp.where(is_valid, padded_shares[picked_index], jnp.float32(0.0))
        return (token_index, expert_out.astype(jnp.float32) * weights_here[:, None])
    token_lists, terms = lax.map(one_expert, jnp.arange(EXPERTS, dtype=jnp.int32))
    total = jnp.zeros((TOKENS + 1, D), jnp.float32).at[token_lists.reshape(-1)].add(terms.reshape(-1, D))
    mixed_out = total[:TOKENS].astype(jnp.bfloat16)
    return (gate_weight, up_weight, down_weight, mixed_out)
```

```python
import functools
import jax
import jax.numpy as jnp
from jax import lax
from jax.experimental import pallas as pl
from jax.experimental.pallas import tpu as pltpu
from jax.sharding import PartitionSpec as P

EPS = 1e-06
NX = 4
NZ = 4
NG = 2
NY = 4
CAP = 48
BF = jnp.bfloat16
F32 = jnp.float32


def shift_x(d):
    return [(z * NX + x, z * NX + (x + d) % NX) for z in range(NZ) for x in range(NX)]


def shift_run(k):
    return [(z * NX + x, ((z + k) % NZ) * NX + x) for z in range(NZ) for x in range(NX)]


def shift_z(d):
    n = NG * NZ
    return [(z * NX + x, ((z + d) % n) * NX + x) for z in range(n) for x in range(NX)]


def shift_tp(d, s):
    return [(y * 2 + c, ((y + d) % NY) * 2 + (c ^ s)) for y in range(NY) for c in range(2)]


def place():
    fs = lax.axis_index("fs")
    return lax.axis_index("gr") * NZ + fs // NX, fs // NX, fs % NX, lax.axis_index("tp")


def call(kernel, outs, args, name, cost=(0, 0), **more):
    size = sum(a.size * a.dtype.itemsize for a in args) + sum(o.size * o.dtype.itemsize for o in outs)
    return pl.pallas_call(
        kernel,
        out_shape=outs,
        name=name,
        cost_estimate=pl.CostEstimate(
            flops=max(int(cost[0]), size * 300), bytes_accessed=size, transcendentals=0
        ),
        **more,
    )(*args)


def shape(dims, dtype=BF):
    return jax.ShapeDtypeStruct(dims, dtype)


VM = pl.BlockSpec(memory_space=pltpu.VMEM)


def cast_kernel(scaled, *refs):
    _, _, x, _ = place()
    if scaled:
        gain, master, outs = refs[0], refs[1], refs[2:]
    else:
        master, outs = refs[0], refs[1:]
    for d in range(NX):
        rows = master[lax.rem(x + d, NX)]
        if scaled:
            rows = rows * gain[...]
        outs[d][0] = rows.astype(BF)


def cast(master, gain):
    e, r, c = master.shape
    specs = [pl.BlockSpec((NX, r, c), lambda i: (i, 0, 0))]
    args = [master]
    if gain is not None:
        specs = [pl.BlockSpec((r, 1), lambda i: (0, 0))] + specs
        args = [gain.reshape(r, 1)] + args
    return call(
        functools.partial(cast_kernel, gain is not None),
        [shape((NZ, r, c))] * NX,
        args,
        "cast",
        grid=(NZ,),
        in_specs=specs,
        out_specs=[pl.BlockSpec((1, r, c), lambda i: (i, 0, 0))] * NX,
    )


def sort_kernel(*refs):
    _, zl, x, _ = place()
    ins, outs = refs[:NX], refs[NX:]
    for k in range(NZ):
        for d in range(NX):
            outs[k][lax.rem(x + NX - d, NX)] = ins[d][lax.rem(zl + k, NZ)]


def spread(master, gain):
    sent = cast(master, gain)
    near = [sent[0]] + [lax.ppermute(sent[d], "fs", shift_x(d)) for d in range(1, NX)]
    _, r, c = master.shape
    blocks = call(
        sort_kernel,
        [shape((NX, r, c))] * NZ,
        near,
        "sort",
        in_specs=[VM] * NX,
        out_specs=[VM] * NZ,
    )
    blocks = [b.reshape(NX * r, c) for b in blocks]
    order = [4, 3, 5, 2, 6, 1, 7]
    pieces = {0: blocks[0]}
    for d in order:
        pieces[d] = lax.ppermute(blocks[d % NZ], ("gr", "fs"), shift_z(d))
    return [pieces[d] for d in range(NG * NZ)]


def fill_kernel(ids_ref, tok_ref, *outs):
    _, zl, x, _ = place()
    ids = ids_ref[...]
    count = ids.shape[1]
    e = NZ * NX
    rel = (((ids // NX) - zl + NZ) % NZ) * NX + (ids - x + NX) % NX
    wide = lax.broadcasted_iota(jnp.int32, (e, count), 0)
    named = (wide == rel[0:1, :]) | (wide == rel[1:2, :])
    before = lax.broadcasted_iota(jnp.int32, (count, count), 0) < lax.broadcasted_iota(
        jnp.int32, (count, count), 1
    )
    rank = jnp.dot(
        named.astype(F32).astype(BF), before.astype(F32).astype(BF), preferred_element_type=F32
    )
    key = jnp.where(named, rank, -1.0)
    slot = lax.broadcasted_iota(jnp.int32, (CAP, count), 0).astype(F32)
    tok = tok_ref[...]
    for k in range(NZ):
        for d in range(NX):
            i = k * NX + d
            pick = (slot == key[i : i + 1, :]).astype(F32).astype(BF)
            outs[k][d] = jnp.dot(pick, tok, preferred_element_type=F32).astype(BF)


def turn_kernel(*refs):
    n = len(refs) // 2
    for a in range(n):
        for b in range(n):
            refs[n + b][a] = refs[a][b]


def turn(arrays):
    return call(
        turn_kernel,
        [shape(arrays[0].shape)] * 4,
        arrays,
        "turn",
        in_specs=[VM] * 4,
        out_specs=[VM] * 4,
    )


def stack_kernel(*refs):
    out = refs[-1]
    for i in range(len(refs) - 1):
        out[i] = refs[i][...]


def gather_tp(piece):
    pieces = {(0, 0): piece}
    for d in (2, 1, 3):
        pieces[d, 0] = lax.ppermute(piece, "tp", shift_tp(d, 0))
    for d in (0, 1, 3, 2):
        pieces[d, 1] = lax.ppermute(pieces[d, 0], "tp", shift_tp(0, 1))
    return [pieces[d, s] for d in range(NY) for s in range(2)]


def tp_from(tp, d, s):
    y, c = tp // 2, lax.rem(tp, 2)
    return lax.rem(y + NY - d, NY) * 2 + (c if s == 0 else 1 - c)


def gate_kernel(*refs):
    z, _, _, tp = place()
    xs, ws, (full, sums, inv) = refs[:8], refs[8:16], refs[16:]
    for d in range(8):
        full[lax.rem(z + 8 - d, 8)] = ws[d][...]
    width = 8 * xs[0].shape[1]
    rows = 256

    def step(m, carry):
        at = pl.ds(pl.multiple_of(m * rows, rows), rows)
        total = jnp.zeros((rows, full.shape[2]), F32)
        squares = jnp.zeros((rows, 1), F32)
        for i in range(8):
            x = xs[i][at, :]
            total += jnp.dot(x, full[tp_from(tp, i // 2, i % 2)], preferred_element_type=F32)
            wide = x.astype(F32)
            squares += jnp.sum(wide * wide, axis=1, keepdims=True)
        r = lax.rsqrt(squares / width + EPS)
        sums[at, :] = total * r * (width**-0.5)
        inv[at, :] = jnp.broadcast_to(r, (rows, 128))
        return carry

    lax.fori_loop(0, xs[0].shape[0] // rows, step, 0)


def up_kernel(*refs):
    z, _, _, tp = place()
    xs, ws, (gate, inv), (full, hidden) = refs[:8], refs[8:16], refs[16:18], refs[18:]
    for d in range(8):
        full[lax.rem(z + 8 - d, 8)] = ws[d][...]
    width = 8 * xs[0].shape[1]
    rows = 256

    def step(m, carry):
        at = pl.ds(pl.multiple_of(m * rows, rows), rows)
        total = jnp.zeros((rows, full.shape[2]), F32)
        for i in range(8):
            total += jnp.dot(
                xs[i][at, :], full[tp_from(tp, i // 2, i % 2)], preferred_element_type=F32
            )
        up = total * inv[at, 0:1] * (width**-0.5)
        g = gate[at, :]
        hidden[at, :] = (g / (1.0 + jnp.exp(-g)) * up).astype(BF)
        return carry

    lax.fori_loop(0, xs[0].shape[0] // rows, step, 0)


def down_kernel(*refs):
    z, _, _, tp = place()
    hs, ws = refs[:8], refs[8:16]
    outs, sends, full = refs[16:20], refs[20:28], refs[28]
    for d in range(8):
        full[lax.rem(z + 8 - d, 8)] = ws[d][...]
    for i in range(8):
        sends[i][...] = full[tp_from(tp, NY - i // 2, i % 2)]
    depth = 8 * hs[0].shape[1]
    rows = outs[0].shape[0]
    for m in range(4):
        total = jnp.zeros((rows, full.shape[2]), F32)
        for i in range(8):
            total += jnp.dot(
                hs[i][m * rows : (m + 1) * rows, :],
                full[tp_from(tp, i // 2, i % 2)],
                preferred_element_type=F32,
            )
        outs[m][...] = (total * depth**-0.5).astype(BF)


def join_kernel(*refs):
    tp = lax.axis_index("tp")
    out = refs[8]
    width = refs[0].shape[1]
    for i in range(8):
        at = pl.multiple_of(tp_from(tp, i // 2, i % 2) * width, width)
        out[:, pl.ds(at, width)] = refs[i][...]


def mix_kernel(ids_ref, logits_ref, *refs):
    _, zl, x, _ = place()
    out = refs[4]
    ids = ids_ref[...]
    count, e = ids.shape[0], NZ * NX
    rel = (((ids // NX) - zl + NZ) % NZ) * NX + (ids - x + NX) % NX
    wide = lax.broadcasted_iota(jnp.int32, (count, e), 1)
    ones = [(wide == rel[:, j : j + 1]).astype(F32) for j in range(2)]
    after = lax.broadcasted_iota(jnp.int32, (count, count), 1) < lax.broadcasted_iota(
        jnp.int32, (count, count), 0
    )
    rank = jnp.dot(
        after.astype(F32).astype(BF), (ones[0] + ones[1]).astype(BF), preferred_element_type=F32
    )
    gates = 1.0 / (1.0 + jnp.exp(-logits_ref[...]))
    shares = gates / (gates[:, 0:1] + gates[:, 1:2])
    span = NX * CAP
    lane = lax.broadcasted_iota(jnp.int32, (count, span), 1).astype(F32)
    mixed = jnp.zeros(out.shape, F32)
    for j in range(2):
        place_j = rel[:, j : j + 1].astype(F32) * CAP + jnp.sum(
            ones[j] * rank, axis=1, keepdims=True
        )
        picked = jnp.zeros(out.shape, F32)
        for k in range(NZ):
            pick = (lane == place_j - float(k * span)).astype(F32).astype(BF)
            picked += jnp.dot(pick, refs[k][...], preferred_element_type=F32)
        mixed += shares[:, j : j + 1] * picked
    out[...] = mixed.astype(BF)


def body(tokens, route_ids, route_logits, gain, gate_master, up_master, down_master):
    count, slice_width = tokens.shape
    experts = gate_master.shape[0]
    hid = gate_master.shape[2]
    total_rows = experts * CAP
    group = NX * CAP

    slots = call(
        fill_kernel,
        [shape((NX, CAP, slice_width))] * NZ,
        [route_ids.T, tokens],
        "fill",
        in_specs=[VM] * 2,
        out_specs=[VM] * NZ,
    )
    came = [slots[0]] + [lax.ppermute(slots[k], "fs", shift_run(k)) for k in range(1, NZ)]
    gate_p = spread(gate_master, gain)
    onward = turn(came)
    here = [onward[0]] + [lax.ppermute(onward[d], "fs", shift_x(d)) for d in range(1, NX)]
    own = call(
        stack_kernel,
        [shape((NX, NZ, CAP, slice_width))],
        here,
        "stack",
        in_specs=[VM] * NX,
        out_specs=[VM],
    )[0].reshape(total_rows, slice_width)
    xs = gather_tp(own)
    up_p = spread(up_master, gain)
    down_p = spread(down_master, None)

    gate_full, gate_sum, inv = call(
        gate_kernel,
        [shape((8,) + gate_p[0].shape), shape((total_rows, hid), F32), shape((total_rows, 128), F32)],
        xs + gate_p,
        "gate",
        in_specs=[VM] * 16,
        out_specs=[VM] * 3,
    )
    up_full, hidden = call(
        up_kernel,
        [shape((8,) + up_p[0].shape), shape((total_rows, hid))],
        xs + up_p + [gate_sum, inv],
        "up",
        in_specs=[VM] * 18,
        out_specs=[VM] * 2,
    )
    hs = gather_tp(hidden)
    res = call(
        down_kernel,
        [shape((group, slice_width))] * 4 + [shape(down_p[0].shape)] * 8,
        hs + down_p,
        "down",
        in_specs=[VM] * 16,
        out_specs=[VM] * 12,
        scratch_shapes=[pltpu.VMEM((8,) + down_p[0].shape, BF)],
    )
    back, sends = res[:4], res[4:]
    back = [back[0]] + [lax.ppermute(back[d], "fs", shift_x(-d)) for d in range(1, NX)]
    landed = [sends[0]] + [
        lax.ppermute(sends[i], "tp", shift_tp(i // 2, i % 2)) for i in range(1, 8)
    ]
    ready = turn([b.reshape(NZ, CAP, slice_width) for b in back])
    ready = [a.reshape(group, slice_width) for a in ready]
    final = [ready[0]] + [lax.ppermute(ready[k], "fs", shift_run(-k)) for k in range(1, NZ)]
    mixed = call(
        mix_kernel,
        [shape((count, slice_width))],
        [route_ids, route_logits] + final,
        "mix",
        in_specs=[VM] * 6,
        out_specs=[VM],
    )[0]
    down_out = call(
        join_kernel,
        [shape((down_p[0].shape[0], 8 * slice_width))],
        landed,
        "join",
        in_specs=[VM] * 8,
        out_specs=[VM],
    )[0]
    return (
        gate_full.reshape(1, -1, hid),
        up_full.reshape(1, -1, hid),
        down_out[None],
        mixed,
    )


def solution(mesh):
    in_specs = (
        P(("gr", "fs"), "tp"),
        P(("gr", "fs"), None),
        P(("gr", "fs"), None),
        P(("gr", "fs")),
        P(None, ("gr", "fs"), "tp"),
        P(None, ("gr", "fs"), "tp"),
        P(None, ("gr", "fs"), "tp"),
    )
    out_specs = (
        P("fs", None, "tp"),
        P("fs", None, "tp"),
        P("fs", "tp", None),
        P(("gr", "fs"), "tp"),
    )
    return jax.shard_map(body, mesh=mesh, in_specs=in_specs, out_specs=out_specs, check_vma=False)
```
